32 devices in a mesh: sp: 16 (over z, y, x), dp: 2 (over core).
Axes of the slice: x: 2, y: 2, z: 4, core: 2. Of those that a mesh axis runs over, the one named last changes fastest.
Arguments:
- tokens: bfloat16 [2, 2048, 2048], P('dp', 'sp'), may hold values from -6 to 6
- w_value: bfloat16 [2048, 1024], P('dp', 'sp'), may hold values from -0.125 to 0.125
- w_gate: bfloat16 [2048, 1024], P('dp', 'sp'), may hold values from -0.125 to 0.125
- w_out: bfloat16 [1024, 2048], P('dp', 'sp'), may hold values from -0.1875 to 0.1875
- conv_taps: bfloat16 [1024, 31], replicated, may hold values from -1 to 1
- norm_gain: float32 [1024], replicated, may hold values from 0.1 to 1.9
- norm_bias: float32 [1024], replicated, may hold values from -3 to 3
Outputs:
- mixed: bfloat16 [2, 2048, 2048], P('dp', 'sp')
The draws below stay inside these ranges and needn't reach their ends.
All inputs are finite; a program needn't handle non-finite values.
Results may differ from the reference program's by a relative error of at most 0.0064.
Values may be sent and summed in bfloat16 or wider, within the bound.
No kernel may reach another device: no remote copies, remote signals or barrier semaphores. Data moves between devices by JAX's collectives and lax.ppermute only.
A program may use at most 64 MiB of HBM per device.

```python
import jax
import jax.numpy as jnp
from jax import lax

D = 2048
CH = 1024
KW = 31
SEQ = 2048
SEQS = 2


def levels(stream_key, shape, shards, smallest, largest):
    gain = 1.0
    for position, blocks in shards:
        heights = jax.random.uniform(jax.random.fold_in(jax.random.fold_in(stream_key, 6), position), (blocks,), jnp.float32, smallest / len(shards), largest / len(shards))
        gain = gain * jnp.repeat(jnp.exp(heights), shape[position] // blocks).reshape((-1,) + (1,) * (len(shape) - 1 - position))
    return gain


def scatter_about(stream_key, dims, deviation, limit, split=(), held_as=jnp.bfloat16):
    entries = deviation * jax.random.normal(stream_key, dims, jnp.float32)
    if split:
        entries = entries * levels(stream_key, dims, split, -0.22, 0.18)
    return jnp.clip(entries, -limit, limit).astype(held_as)


def setup_inputs(seed: int = 0) -> dict:
    key_list = jax.random.split(jax.random.key(seed), 8)
    tokens = scatter_about(key_list[0], (SEQS, SEQ, D), 1.0, 6.0, ((0, 2), (1, 16)))
    w_value = scatter_about(key_list[1], (D, CH), D ** -0.5, 0.125, ((0, 2), (1, 16)))
    w_gate = scatter_about(key_list[2], (D, CH), D ** -0.5, 0.125, ((0, 2), (1, 16)))
    w_out = scatter_about(key_list[3], (CH, D), CH ** -0.5, 0.1875, ((0, 2), (1, 16)))
    conv_taps = scatter_about(key_list[4], (CH, KW), KW ** -0.5, 1.0)
    norm_gain = jnp.clip(1.0 + 0.18 * jax.random.normal(key_list[5], (CH,), jnp.float32), 0.1, 1.9)
    norm_bias = scatter_about(key_list[6], (CH,), 0.5, 3.0, (), jnp.float32)
    return {"tokens": tokens, "w_value": w_value, "w_gate": w_gate, "w_out": w_out, "conv_taps": conv_taps, "norm_gain": norm_gain, "norm_bias": norm_bias}


def reference(tokens, w_value, w_gate, w_out, conv_taps, norm_gain, norm_bias):
    margin = KW // 2
    taps = conv_taps.astype(jnp.float32).T

    def one_sequence(seq_rows):
        value = jnp.dot(seq_rows, w_value, preferred_element_type=jnp.float32)
        gate = jnp.dot(seq_rows, w_gate, preferred_element_type=jnp.float32)
        gated = lax.optimization_barrier((value * jax.nn.sigmoid(gate)).astype(jnp.bfloat16))
        padded = jnp.pad(gated, ((margin, margin), (0, 0))).astype(jnp.float32)
        total = jnp.zeros((SEQ, CH), jnp.float32)
        for offset in range(KW):
            total = total + padded[offset:offset + SEQ] * taps[offset][None, :]
        conv = lax.optimization_barrier(total.astype(jnp.bfloat16)).astype(jnp.float32)
        mean = lax.optimization_barrier(jnp.mean(conv, axis=-1, keepdims=True))
        centred = conv - mean
        variance = lax.optimization_barrier(jnp.mean(centred * centred, axis=-1, keepdims=True))
        normed = centred * lax.rsqrt(variance + 1e-05) * norm_gain[None, :] + norm_bias[None, :]
        act = (normed * jax.nn.sigmoid(normed)).astype(jnp.bfloat16)
        return jnp.dot(act, w_out, preferred_element_type=jnp.float32).astype(jnp.bfloat16)
    return lax.map(one_sequence, tokens)
```

```python
import functools

import jax
import jax.numpy as jnp
from jax import lax
from jax.experimental import pallas as pl
from jax.experimental.pallas import tpu as pltpu
from jax.sharding import PartitionSpec as P


PLANE = 4
EDGE = 16
MIB = 1 << 20


def padded_2(block, sides, width):
    for axis, dim in sides:
        count = lax.axis_size(axis)
        forward = [(i, i + 1) for i in range(count - 1)]
        backward = [(target, source) for source, target in forward]
        low = lax.ppermute(
            lax.slice_in_dim(block, block.shape[dim] - width, None, axis=dim), axis, forward
        )
        high = lax.ppermute(lax.slice_in_dim(block, 0, width, axis=dim), axis, backward)
        block = jnp.concatenate([low, block, high], axis=dim)
    return block


def depthwise(padded, taps, length):
    weights = taps.astype(jnp.float32)
    total = jnp.zeros((padded.shape[0], length), jnp.float32)
    for offset in range(taps.shape[1]):
        total = total + weights[:, offset : offset + 1] * padded[
            :, offset : offset + length
        ].astype(jnp.float32)
    return total.astype(jnp.bfloat16)


def normalize(conv_tok, norm_gain, norm_bias):
    values = lax.optimization_barrier(conv_tok).astype(jnp.float32)
    mean = jnp.mean(values, axis=0, keepdims=True)
    centred = values - mean
    variance = jnp.mean(centred * centred, axis=0, keepdims=True)
    normed = centred * lax.rsqrt(variance + 1e-05) * norm_gain[:, None] + norm_bias[:, None]
    return (normed * jax.nn.sigmoid(normed)).astype(jnp.bfloat16)


def gather_weights(tokens, w_value, w_gate, w_out, conv_taps, norm_gain, norm_bias):
    rows = tokens[0]
    contract_rows = (((0,), (1,)), ((), ()))
    contract_first = (((0,), (0,)), ((), ()))
    value_cols, gate_cols, out_cols = (
        lax.all_gather(w_value, "dp", axis=0, tiled=True),
        lax.all_gather(w_gate, "dp", axis=0, tiled=True),
        lax.all_gather(w_out, "dp", axis=0, tiled=True),
    )
    pieces = lax.all_gather((value_cols, gate_cols), "sp", axis=1, tiled=True)
    value = lax.dot_general(pieces[0], rows, contract_rows, preferred_element_type=jnp.float32)
    gate = lax.dot_general(pieces[1], rows, contract_rows, preferred_element_type=jnp.float32)
    gated_t = (value * jax.nn.sigmoid(gate)).astype(jnp.bfloat16)
    margin = conv_taps.shape[1] // 2
    padded = padded_2(gated_t, (("sp", 1),), margin)
    conv_tok = depthwise(padded, conv_taps, gated_t.shape[1])
    act_t = normalize(conv_tok, norm_gain, norm_bias)
    mixed = lax.dot_general(
        act_t,
        lax.all_gather(out_cols, "sp", axis=1, tiled=True),
        contract_first,
        preferred_element_type=jnp.float32,
    )
    return mixed.astype(jnp.bfloat16)[None]


def nt_dot(a, b):
    return lax.dot_general(a, b, (((1,), (1,)), ((), ())), preferred_element_type=jnp.float32)


def project_kernel(place, *refs, rows, wide, half, taps_count):
    tok, refs = refs[:PLANE], refs[PLANE:]
    edges, refs = refs[:PLANE], refs[PLANE:]
    own, refs = refs[:PLANE], refs[PLANE:]
    other, refs = refs[:PLANE], refs[PLANE:]
    taps, refs = refs[0], refs[1:]
    outs, refs = refs[:PLANE], refs[PLANE:]
    wv, wg, gated, shifted = refs
    j, z, c = place[0], place[1], place[2]
    for k in range(PLANE):
        at = pl.ds(pl.multiple_of(((z ^ k) ^ (2 * c)) * wide, wide), wide)
        for side, block in ((c, own[k]), (1 - c, other[k])):
            cols = pl.ds(pl.multiple_of(side * half, half), half)
            wv[at, cols] = block[0:wide, :]
            wg[at, cols] = block[wide : 2 * wide, :]
    low = jnp.zeros((EDGE, 2 * half), jnp.bfloat16)
    high = low
    for d in range(PLANE):
        low = jnp.where(j == (PLANE - 1) ^ d, edges[d][...], low)
        high = jnp.where(j == d, edges[d][...], high)

    def gate_rows(x, at):
        value = nt_dot(x, wv[...])
        gate = nt_dot(x, wg[...])
        gated[at, :] = (value * jax.nn.sigmoid(gate)).astype(jnp.bfloat16).astype(jnp.float32)

    for d in range(PLANE):
        start = pl.multiple_of((j ^ d) * rows + EDGE, EDGE)
        gate_rows(tok[d][...], pl.ds(start, rows))
    ends = jnp.concatenate([low, high], axis=0)
    value = nt_dot(ends, wv[...])
    gate = nt_dot(ends, wg[...])
    ends = (value * jax.nn.sigmoid(gate)).astype(jnp.bfloat16).astype(jnp.float32)
    gated[0:EDGE, :] = ends[0:EDGE]
    gated[PLANE * rows + EDGE : PLANE * rows + 2 * EDGE, :] = ends[EDGE:]

    margin = taps_count // 2
    total_rows = PLANE * rows + 2 * EDGE
    lanes = gated.shape[1]
    for s in range(8):
        if s == 0:
            continue
        for l in range(0, lanes, 128):
            shifted[s - 1, 0 : total_rows - 8, l : l + 128] = gated[
                s : s + total_rows - 8, l : l + 128
            ]
    chunk = 32
    for d in range(PLANE):
        base = (j ^ d) * rows

        @pl.loop(0, rows // chunk)
        def _(i):
            for l in range(0, lanes, 128):
                total = jnp.zeros((chunk, 128), jnp.float32)
                for tap in range(taps_count):
                    reach = tap + EDGE - margin
                    at = pl.ds(pl.multiple_of(base + i * chunk + (reach // 8) * 8, 8), chunk)
                    if reach % 8:
                        piece = shifted[reach % 8 - 1, at, l : l + 128]
                    else:
                        piece = gated[at, l : l + 128]
                    total = total + taps[tap : tap + 1, l : l + 128] * piece
                outs[d][pl.ds(pl.multiple_of(i * chunk, chunk), chunk), l : l + 128] = total.astype(
                    jnp.bfloat16
                )


def project(place, tok, edges, own, other, taps, rows, wide, half, taps_count):
    channels = PLANE * wide
    vmem = pl.BlockSpec(memory_space=pltpu.VMEM)
    total_rows = PLANE * rows + 2 * EDGE
    return pl.pallas_call(
        functools.partial(
            project_kernel, rows=rows, wide=wide, half=half, taps_count=taps_count
        ),
        out_shape=[jax.ShapeDtypeStruct((rows, channels), jnp.bfloat16)] * PLANE,
        in_specs=[pl.BlockSpec(memory_space=pltpu.SMEM)] + [vmem] * (4 * PLANE + 1),
        out_specs=[vmem] * PLANE,
        scratch_shapes=[
            pltpu.VMEM((channels, 2 * half), jnp.bfloat16),
            pltpu.VMEM((channels, 2 * half), jnp.bfloat16),
            pltpu.VMEM((total_rows, channels), jnp.float32),
            pltpu.VMEM((7, total_rows, channels), jnp.float32),
        ],
        compiler_params=pltpu.CompilerParams(vmem_limit_bytes=20 * MIB),
        cost_estimate=pl.CostEstimate(
            flops=4 * total_rows * channels * 2 * half,
            bytes_accessed=8 * MIB,
            transcendentals=total_rows * channels,
        ),
        name="project",
    )(place, *tok, *edges, *own, *other, taps)


def mix_kernel(place, *refs, rows, wide):
    conv, refs = refs[:PLANE], refs[PLANE:]
    gain, bias, refs = refs[0], refs[1], refs[2:]
    own, refs = refs[: 2 * PLANE], refs[2 * PLANE :]
    other, refs = refs[: 2 * PLANE], refs[2 * PLANE :]
    out = refs[0]
    j, z = place[0], place[1]
    values = [conv[d][...].astype(jnp.float32) for d in range(PLANE)]
    count = PLANE * PLANE * wide
    mean = sum(jnp.sum(v, axis=1, keepdims=True) for v in values) / count
    centred = [v - mean for v in values]
    variance = sum(jnp.sum(v * v, axis=1, keepdims=True) for v in centred) / count
    scale = lax.rsqrt(variance + 1e-05)
    acts = []
    for d in range(PLANE):
        normed = centred[d] * scale * gain[d : d + 1, :] + bias[d : d + 1, :]
        acts.append((normed * jax.nn.sigmoid(normed)).astype(jnp.bfloat16))
    act = jnp.concatenate(acts, axis=1)
    cols = out.shape[1] // (PLANE * PLANE)
    for d in range(PLANE):
        for pair in range(2):
            mine, theirs = own[2 * d + pair], other[2 * d + pair]
            both = []
            for e in range(2):
                pieces = []
                for s in range(PLANE):
                    start = (j ^ s) * wide
                    for block in (mine, theirs):
                        for part in range(2):
                            at = pl.multiple_of(start + part * PLANE * wide, wide)
                            pieces.append(block[e, pl.ds(at, wide), :])
                both.append(jnp.concatenate(pieces, axis=0))
            weights = jnp.concatenate(both, axis=1)
            result = jnp.dot(act, weights, preferred_element_type=jnp.float32)
            result = result.astype(jnp.bfloat16)
            for e in range(2):
                k = 2 * pair + e
                at = pl.multiple_of(((z ^ k) * PLANE + (j ^ d)) * cols, cols)
                out[:, pl.ds(at, cols)] = result[:, e * cols : (e + 1) * cols]


def mix(place, conv, gain, bias, own, other, rows, wide, width):
    vmem = pl.BlockSpec(memory_space=pltpu.VMEM)
    return pl.pallas_call(
        functools.partial(mix_kernel, rows=rows, wide=wide),
        out_shape=jax.ShapeDtypeStruct((rows, width), jnp.bfloat16),
        in_specs=[pl.BlockSpec(memory_space=pltpu.SMEM)] + [vmem] * (PLANE + 2 + 4 * PLANE),
        out_specs=vmem,
        compiler_params=pltpu.CompilerParams(vmem_limit_bytes=16 * MIB),
        cost_estimate=pl.CostEstimate(
            flops=2 * rows * width * PLANE * PLANE * wide,
            bytes_accessed=6 * MIB,
            transcendentals=rows * PLANE * PLANE * wide,
        ),
        name="mix",
    )(place, *conv, gain, bias, *own, *other)


def by_planes(tokens, w_value, w_gate, w_out, conv_taps, norm_gain, norm_bias):
    count, cores = lax.axis_size("sp"), lax.axis_size("dp")
    planes = count // PLANE
    rows_in = tokens[0]
    rows, depth = rows_in.shape
    half, wide = w_value.shape
    taps_count = conv_taps.shape[1]
    sp, c = lax.axis_index("sp"), lax.axis_index("dp")
    z, j = sp // PLANE, sp % PLANE
    place = jnp.stack([j, z, c]).astype(jnp.int32)

    def in_plane(x, d):
        return lax.ppermute(x, "sp", [(i, i ^ d) for i in range(count)])

    def across(x, k):
        return lax.ppermute(x, "sp", [(i, i ^ (k * PLANE)) for i in range(count)])

    def core(x):
        return lax.ppermute(x, "dp", [(i, i ^ 1) for i in range(cores)])

    def edge(x, d):
        pairs = []
        for plane in range(planes):
            if plane + 1 < planes:
                pairs.append((plane * PLANE + PLANE - 1, (plane + 1) * PLANE + (PLANE - 1) ^ d))
            if plane > 0:
                pairs.append((plane * PLANE, (plane - 1) * PLANE + d))
        return lax.ppermute(x, "sp", pairs)

    vg = jnp.concatenate([w_value.T, w_gate.T], axis=0)
    tok = [rows_in] + [in_plane(rows_in, d) for d in (1, 2, 3)]
    own_vg = [vg] + [across(vg, k) for k in (1, 2, 3)]
    other_vg = [core(x) for x in own_vg]
    ends = jnp.where(j == 0, rows_in[:EDGE], rows_in[-EDGE:])
    edges = [edge(ends, d) for d in range(PLANE)]

    order = jnp.arange(PLANE) ^ (2 * c)
    which = order * PLANE + j
    taps = conv_taps.T.astype(jnp.float32).reshape(taps_count, -1, wide)[:, which, :]
    taps = taps.reshape(taps_count, PLANE * wide)
    which = order[None, :] * PLANE + (j ^ jnp.arange(PLANE))[:, None]
    gain = norm_gain.reshape(-1, wide)[which].reshape(PLANE, PLANE * wide)
    bias = norm_bias.reshape(-1, wide)[which].reshape(PLANE, PLANE * wide)

    out_z = [w_out] + [across(w_out, k) for k in (1, 2, 3)]
    pairs = [jnp.stack(out_z[:2]), jnp.stack(out_z[2:])]
    near = [in_plane(p, 1) for p in pairs]
    far = [in_plane(p, 2) for p in pairs]
    third = [in_plane(near[0], 2), in_plane(far[1], 1)]
    own_out = [*pairs, *near, *far, *third]
    other_out = [core(x) for x in own_out]

    blocks = project(place, tok, edges, own_vg, other_vg, taps, rows, wide, half, taps_count)
    conv = [blocks[0]] + [in_plane(blocks[d], d) for d in (1, 2, 3)]
    return mix(place, conv, gain, bias, own_out, other_out, rows, wide, depth)[None]


def solution(mesh):
    in_specs = (P("dp", "sp", None), P("dp", "sp"), P("dp", "sp"), P("dp", "sp"), P(), P(), P())
    out_specs = P("dp", "sp", None)
    planar = mesh.shape["sp"] == PLANE * PLANE and mesh.shape["dp"] == 2
    return jax.shard_map(
        by_planes if planar else gather_weights,
        mesh=mesh,
        in_specs=in_specs,
        out_specs=out_specs,
        check_vma=False,
    )
```
